32 devices in a mesh: grp: 2 (over y), kv: 4 (over z), tp: 4 (over x, core).
Axes of the slice: x: 2, y: 2, z: 4, core: 2. Of those that a mesh axis runs over, the one named last changes fastest.
Arguments:
- tokens: bfloat16 [24, 4096], P('grp', 'kv'), parts along dimension 0, may hold values from -25 to 25
- mix_gain: bfloat16 [4096], P('kv'), may hold values from 0.099609375 to 1.8984375
- query_weight: bfloat16 [4096, 2048], P('kv', 'tp'), may hold values from -0.09375 to 0.09375
- key_weight: bfloat16 [4096, 2048], P('kv', 'tp'), may hold values from -0.09375 to 0.09375
- decay_weight: bfloat16 [4096, 2048], P('kv', 'tp'), may hold values from -0.09375 to 0.09375
- value_weight: bfloat16 [4096, 4096], P('kv', 'tp'), may hold values from -0.09375 to 0.09375
- gate_weight: bfloat16 [4096, 4096], P('kv', 'tp'), may hold values from -0.09375 to 0.09375
- state: float32 [24, 8, 256, 512], P(('grp', 'kv'), 'tp'), parts along dimension 0, may hold values from -6 to 6
- block_keys: bfloat16 [24, 64, 2048], P(('grp', 'kv'), None, 'tp'), parts along dimension 0, may hold values from -6 to 6
- block_values: bfloat16 [24, 64, 4096], P(('grp', 'kv'), None, 'tp'), parts along dimension 0, may hold values from -6 to 6
- block_decay: float32 [24, 64, 2048], P(('grp', 'kv'), None, 'tp'), parts along dimension 0, as said below
- lengths: int32 [24], P(('grp', 'kv')), parts along dimension 0, may hold values from 1 to 64, 384 in all
- head_gain: bfloat16 [512], replicated, may hold values from 0.099609375 to 1.8984375
- out_weight: bfloat16 [4096, 4096], P('tp', 'kv'), may hold values from -0.09375 to 0.09375
- mlp_gain: bfloat16 [4096], P('kv'), may hold values from 0.099609375 to 1.8984375
- up_weight: bfloat16 [4096, 16384], P('kv', 'tp'), may hold values from -0.09375 to 0.09375
- down_weight: bfloat16 [16384, 4096], P('tp', 'kv'), may hold values from -0.046875 to 0.046875
Outputs:
- result: bfloat16 [24, 4096], P('grp', 'kv'), parts along dimension 0
The draws below stay inside these ranges and needn't reach their ends.
There are 2 independent parts, one for each index of `grp`. The reference program is written for one: setup_inputs(seed, part) draws one part's arguments, and reference() takes and returns one part's arrays. A program takes and returns all parts, laid end to end along the dimension named above; an argument that names none is the same for every part. Nothing has to cross between parts.
Inputs may be any that keep to these rules, and one draw needn't show every extreme that they name: `block_decay`: along a row's block positions the values never rise. In each part the 12 lengths add up to 384, and the largest is 64.
All inputs are finite; a program needn't handle non-finite values. No bound on the sum of `lengths` on one device may be relied on, other than what follows from the above.
Results may differ from the reference program's by a relative error of at most 0.0062.
Values may be sent and summed in bfloat16 or wider, within the bound.
A program may use at most 64 MiB of HBM per device.

```python
import math
import jax
import jax.numpy as jnp
import numpy as np
from jax import lax

D = 4096
HEAD_TOTAL = 8
HEAD_KEY_WIDTH = 256
HV = 512
FF = 16384
BLOCK_POSITIONS = 64
KEY_CHANNELS = 2048
DV = 4096
GROUP_SEQUENCES = 12


def draw_tokens(key, part):
    key_rows = jax.random.split(jax.random.fold_in(key, 11), 3)
    column_pos = jnp.arange(D, dtype=jnp.float32) / D - 0.5
    random_wobble = jnp.exp(jax.random.uniform(key_rows[1], (D,), jnp.float32, -0.3, 0.3))
    column_scale = 3.0 ** column_pos * random_wobble
    row_scale = 3.0 ** jax.random.uniform(key_rows[2], (GROUP_SEQUENCES, 1), jnp.float32, -0.5, 0.5)
    entries = jax.random.truncated_normal(key_rows[0], -6.0, 6.0, (GROUP_SEQUENCES, D), jnp.float32)
    return (entries * column_scale[None, :] * row_scale).astype(jnp.bfloat16)


def draw_block_decay(key, part):
    key_rows = jax.random.split(jax.random.fold_in(key, 23), 7)
    slow_share = 0.5
    slow_mask = jax.random.uniform(key_rows[0], (KEY_CHANNELS,), jnp.float32) < slow_share
    slow_rate = jnp.exp(jax.random.uniform(key_rows[1], (KEY_CHANNELS,), jnp.float32, math.log(0.05), 0.0)) / BLOCK_POSITIONS
    fast_rate = jnp.exp(jax.random.uniform(key_rows[2], (KEY_CHANNELS,), jnp.float32, math.log(4.0), math.log(8.0))) / BLOCK_POSITIONS
    channel_decay_rate = jnp.where(slow_mask, slow_rate, fast_rate)
    sequence_factor = jnp.exp(jax.random.uniform(key_rows[3], (GROUP_SEQUENCES, 1, 1), jnp.float32, -0.7, 0.7))
    random_wobble = jax.random.uniform(key_rows[4], (GROUP_SEQUENCES, BLOCK_POSITIONS, KEY_CHANNELS), jnp.float32, 0.5, 1.5)
    spike_mask = jax.random.uniform(key_rows[5], (GROUP_SEQUENCES, BLOCK_POSITIONS, HEAD_TOTAL, 1), jnp.float32) < 2.0 / BLOCK_POSITIONS
    retained_fraction = jax.random.uniform(key_rows[6], (GROUP_SEQUENCES, BLOCK_POSITIONS, HEAD_TOTAL, 1), jnp.float32, 0.5, 0.8)
    spike_draw = jnp.where(spike_mask, jnp.log(retained_fraction), 0.0)
    spike_draw = jnp.broadcast_to(spike_draw, (GROUP_SEQUENCES, BLOCK_POSITIONS, HEAD_TOTAL, HEAD_KEY_WIDTH)).reshape(GROUP_SEQUENCES, BLOCK_POSITIONS, KEY_CHANNELS)
    length_increments = -channel_decay_rate[None, None, :] * sequence_factor * random_wobble + spike_draw
    return jnp.cumsum(length_increments, axis=1).astype(jnp.float32)


def steps_of(stream_key, extent, shards, least, largest):
    gain, own = 1.0, jax.random.fold_in(stream_key, 6)
    for axis_at, shards_of in shards:
        steps = jnp.exp(jax.random.uniform(jax.random.fold_in(own, axis_at), (shards_of,), jnp.float32, least / len(shards), largest / len(shards)))
        gain = gain * jnp.repeat(steps, extent[axis_at] // shards_of).reshape([-1 if axis == axis_at else 1 for axis in range(len(extent))])
    return gain


def length_profile(amount, total, limit, slope):
    weights = [(1 << 20) // math.isqrt(rank ** slope) + 1 for rank in range(2, amount + 1)]
    surplus, counts = total - limit - (amount - 1), [1] * (amount - 1)
    while surplus > 0:
        candidates = [i for i in range(amount - 1) if counts[i] < limit]
        pool, budget = sum([weights[i] for i in candidates]), surplus
        for i in candidates:
            addition = min(limit - counts[i], max(1, budget * weights[i] // pool), surplus)
            counts[i] = counts[i] + addition
            surplus = surplus - addition
    return np.array([limit] + counts)


def uneven(rng, count, total, bound, skew):
    if count == 2:
        one = jax.random.randint(rng, (), max(1, total - bound), min(bound, total - 1) + 1)
        return jnp.stack([one, total - one])
    tallies = jnp.asarray(length_profile(count, total, bound, skew), jnp.int32)
    pairs = (count - 1) // 2
    source_of, sink = tallies[1:1 + 2 * pairs:2], tallies[2:2 + 2 * pairs:2]
    margin = jnp.minimum(source_of - 1, bound - sink)
    passed = jax.random.randint(jax.random.fold_in(rng, 1), (pairs,), 0, 1 << 20) % (margin + 1)
    tallies = tallies.at[1:1 + 2 * pairs:2].set(source_of - passed).at[2:2 + 2 * pairs:2].set(sink + passed)
    return tallies[jax.random.permutation(jax.random.fold_in(rng, 2), count)]


def normal_values(rng, extent, width, limit, cuts=(), kind=jnp.bfloat16):
    level = steps_of(rng, extent, cuts, -0.22, 0.18) if cuts else 1.0
    values = jax.random.normal(rng, extent, jnp.float32) * width * level
    return jnp.minimum(jnp.maximum(values, -limit), limit).astype(kind)


def setup_inputs(seed: int = 0, part: int = 0) -> dict:
    seeds = jax.random.split(jax.random.key(seed), 18)
    own_keys = jax.random.split(jax.random.fold_in(seeds[17], part), 18)
    tokens = draw_tokens(jax.random.fold_in(jax.random.fold_in(seeds[17], part), 71), part)
    mix_gain = jnp.clip(1.0 + 0.18 * jax.random.normal(seeds[1], (D,), jnp.float32), 0.099609375, 1.8984375).astype(jnp.bfloat16)
    query_weight = normal_values(seeds[2], (D, KEY_CHANNELS), D ** -0.5, 0.09375, ((0, 4), (1, 4)))
    key_weight = normal_values(seeds[3], (D, KEY_CHANNELS), D ** -0.5, 0.09375, ((0, 4), (1, 4)))
    decay_weight = normal_values(seeds[4], (D, KEY_CHANNELS), D ** -0.5, 0.09375, ((0, 4), (1, 4)))
    value_weight = normal_values(seeds[5], (D, DV), D ** -0.5, 0.09375, ((0, 4), (1, 4)))
    gate_weight = normal_values(seeds[6], (D, DV), D ** -0.5, 0.09375, ((0, 4), (1, 4)))
    state = normal_values(own_keys[7], (GROUP_SEQUENCES, HEAD_TOTAL, HEAD_KEY_WIDTH, HV), 1.0, 6.0, ((0, 4), (1, 4)), jnp.float32)
    block_keys = normal_values(own_keys[8], (GROUP_SEQUENCES, BLOCK_POSITIONS, KEY_CHANNELS), 1.0, 6.0, ((0, 4), (2, 4)))
    block_values = normal_values(own_keys[9], (GROUP_SEQUENCES, BLOCK_POSITIONS, DV), 1.0, 6.0, ((0, 4), (2, 4)))
    block_decay = draw_block_decay(jax.random.fold_in(jax.random.fold_in(seeds[17], part), 71), part)
    lengths = uneven(own_keys[11], GROUP_SEQUENCES, BLOCK_POSITIONS * GROUP_SEQUENCES // 2, BLOCK_POSITIONS, 2).astype(jnp.int32)
    head_gain = jnp.clip(1.0 + 0.18 * jax.random.normal(seeds[12], (HV,), jnp.float32), 0.099609375, 1.8984375).astype(jnp.bfloat16)
    out_weight = normal_values(seeds[13], (DV, D), DV ** -0.5, 0.09375, ((0, 4), (1, 4)))
    mlp_gain = jnp.clip(1.0 + 0.18 * jax.random.normal(seeds[14], (D,), jnp.float32), 0.099609375, 1.8984375).astype(jnp.bfloat16)
    up_weight = normal_values(seeds[15], (D, FF), D ** -0.5, 0.09375, ((0, 4), (1, 4)))
    down_weight = normal_values(seeds[16], (FF, D), FF ** -0.5, 0.046875, ((0, 4), (1, 4)))
    return {"tokens": tokens, "mix_gain": mix_gain, "query_weight": query_weight, "key_weight": key_weight, "decay_weight": decay_weight, "value_weight": value_weight, "gate_weight": gate_weight, "state": state, "block_keys": block_keys, "block_values": block_values, "block_decay": block_decay, "lengths": lengths, "head_gain": head_gain, "out_weight": out_weight, "mlp_gain": mlp_gain, "up_weight": up_weight, "down_weight": down_weight}


HIGHEST = lax.Precision.HIGHEST
EPSILON = 1e-06

def attend(query, key, value, log_decay, state, keys_cached, values_cached, decay_cached, lengths):
    block_len = keys_cached.shape[1]
    position = jnp.arange(block_len, dtype=jnp.int32)
    live = position[None, :] < lengths[:, None]
    latest = position[None, :] == lengths[:, None] - 1
    before = lax.optimization_barrier(jnp.sum(jnp.where(latest[:, :, None, None], decay_cached, 0.0), axis=1))
    current = before + log_decay
    carried = jnp.einsum('shc,shcv->shv', query * jnp.exp(current), state, precision=HIGHEST)
    spread = jnp.where(live[:, :, None, None], current[:, None] - decay_cached, -jnp.inf)
    weighted = jnp.exp(spread) * keys_cached.astype(jnp.float32)
    scores = jnp.einsum('shc,sbhc->sbh', query, weighted, precision=HIGHEST)
    inner = jnp.einsum('sbh,sbhv->shv', scores, values_cached.astype(jnp.float32), precision=HIGHEST)
    own = lax.optimization_barrier(jnp.sum(query * key, axis=-1, keepdims=True)) * value
    return carried + inner + own

def reference(tokens, mix_gain, query_weight, key_weight, decay_weight, value_weight, gate_weight, state, block_keys, block_values, block_decay, lengths, head_gain, out_weight, mlp_gain, up_weight, down_weight):
    rows = tokens.shape[0]
    tok_float = tokens.astype(jnp.float32)
    inverse = lax.rsqrt(lax.optimization_barrier(jnp.mean(tok_float * tok_float, axis=1)) + EPSILON)[:, None]
    scaled = (tok_float * mix_gain.astype(jnp.float32)).astype(jnp.bfloat16)
    query = jnp.dot(scaled, query_weight, preferred_element_type=jnp.float32) * inverse * HEAD_KEY_WIDTH ** (-0.5)
    key = jnp.dot(scaled, key_weight, preferred_element_type=jnp.float32) * inverse
    decay_in = jnp.dot(scaled, decay_weight, preferred_element_type=jnp.float32) * inverse
    value = jnp.dot(scaled, value_weight, preferred_element_type=jnp.float32) * inverse
    gate = jnp.dot(scaled, gate_weight, preferred_element_type=jnp.float32) * inverse
    log_decay = jax.nn.log_sigmoid(decay_in) / 16.0
    block_len = block_keys.shape[1]
    attended = attend(query.reshape(rows, HEAD_TOTAL, HEAD_KEY_WIDTH), key.reshape(rows, HEAD_TOTAL, HEAD_KEY_WIDTH), value.reshape(rows, HEAD_TOTAL, HV), log_decay.reshape(rows, HEAD_TOTAL, HEAD_KEY_WIDTH), state, block_keys.reshape(rows, block_len, HEAD_TOTAL, HEAD_KEY_WIDTH), block_values.reshape(rows, block_len, HEAD_TOTAL, HV), block_decay.reshape(rows, block_len, HEAD_TOTAL, HEAD_KEY_WIDTH), lengths)
    normed = attended * lax.rsqrt(lax.optimization_barrier(jnp.mean(attended * attended, axis=-1, keepdims=True)) + EPSILON)
    normed = normed * head_gain.astype(jnp.float32) * jax.nn.silu(gate.reshape(rows, HEAD_TOTAL, HV))
    merged = normed.reshape(rows, HEAD_TOTAL * HV).astype(jnp.bfloat16)
    mixed = (tok_float + jnp.dot(merged, out_weight, preferred_element_type=jnp.float32)).astype(jnp.bfloat16)
    mixed_float = mixed.astype(jnp.float32)
    inverse_mlp = lax.rsqrt(lax.optimization_barrier(jnp.mean(mixed_float * mixed_float, axis=1)) + EPSILON)[:, None]
    scaled_mlp = (mixed_float * mlp_gain.astype(jnp.float32)).astype(jnp.bfloat16)
    preact = jnp.dot(scaled_mlp, up_weight, preferred_element_type=jnp.float32) * inverse_mlp
    squared = jnp.square(jax.nn.relu(preact)).astype(jnp.bfloat16)
    return (mixed_float + jnp.dot(squared, down_weight, preferred_element_type=jnp.float32)).astype(jnp.bfloat16)
```

```python
import functools

import jax
import jax.numpy as jnp
from jax import lax
from jax.experimental import pallas as pl
from jax.experimental.pallas import tpu as pltpu
from jax.sharding import PartitionSpec as P

EPSILON = 1e-06
MESH = pl.DeviceIdType.MESH
F32, BF16 = jnp.float32, jnp.bfloat16
ANY = pl.BlockSpec(memory_space=pl.ANY)


def kernel(
    cfg,
    tokens, mix_gain, wq, wk, wd, wv, wg, state, keys, values, decay, lengths,
    head_gain, wo, mlp_gain, wu, wdn,
    out,
    tok_v, mix_v, wq_v, wk_v, wd_v, wv_v, wg_v, state_v, keys_v, values_v, decay_v, len_s,
    hg_v, wo_v, mg_v, wu_v, wdn_v,
    slab_a, slab_v, slab_g, recv_a, recv_v, recv_g, gath, outx, sq_own, sq_recv, mlp_lhs,
    up_send, up_recv, sq_mine, sq_all, acc, downx, mat,
    load_sem, send_sem, recv_sem, c_r,
):
    n_kv, n_tp, width, S, SP, rs, gs, halves = cfg
    rows, depth = tok_v.shape
    heads, hk, hv = state_v.shape[1:]
    positions = keys_v.shape[1]
    kcols = wq_v.shape[1]
    vcols = wv_v.shape[1]
    rr, cw = up_send.shape[1] * gs, up_send.shape[3]
    dh = depth // halves
    me = lax.axis_index("kv")
    mt = lax.axis_index("tp")

    loads = {}
    pairs = [
        (tokens, tok_v, 0), (mix_gain, mix_v, 16), (wq, wq_v, 1), (wk, wk_v, 2), (wd, wd_v, 3),
        (wv, wv_v, 4), (wg, wg_v, 5), (lengths, len_s, 6), (decay, decay_v, 7), (keys, keys_v, 8),
        (values, values_v, 9), (state, state_v, 10), (head_gain, hg_v, 11), (wo, wo_v, 12),
        (mlp_gain, mg_v, 13), (wu, wu_v, 14), (wdn, wdn_v, 15),
    ]
    for src, dst, at in pairs:
        copy = pltpu.make_async_copy(src, dst, load_sem.at[at])
        copy.start()
        loads[id(dst)] = copy

    def ready(ref):
        loads[id(ref)].wait()

    def wait_for(ref, sem):
        pltpu.make_async_copy(ref, ref, sem).wait()

    half = n_kv // 2
    low = me < half

    def kv_peer(k):
        if n_kv % 2:
            return lax.rem(me + k + 1, n_kv)
        if k < half:
            return jnp.where(low, n_kv - 1 - k, k)
        base = jnp.where(low, 0, half)
        return base + lax.rem(me - base + (k - half + 1), half)

    barrier = pltpu.get_barrier_semaphore()
    for d in range(1, n_kv):
        pl.semaphore_signal(barrier, inc=1, device_id={"kv": lax.rem(me + d, n_kv)}, device_id_type=MESH)
    for d in range(1, n_tp):
        pl.semaphore_signal(barrier, inc=1, device_id={"tp": lax.rem(mt + d, n_tp)}, device_id_type=MESH)

    sent = []

    def size_of(ref):
        size = jnp.dtype(ref.dtype).itemsize
        for n in ref.shape:
            size *= n
        return size

    def send_kv(src, dst, recv, peer, count=1):
        pltpu.make_async_remote_copy(
            src_ref=src, dst_ref=dst, send_sem=send_sem.at[0], recv_sem=recv,
            device_id={"kv": peer}, device_id_type=MESH).start()
        sent.append(count * size_of(src))

    def send_tp(src, dst, recv, d):
        pltpu.make_async_remote_copy(
            src_ref=src, dst_ref=dst, send_sem=send_sem.at[0], recv_sem=recv,
            device_id={"tp": lax.rem(mt + d, n_tp)}, device_id_type=MESH).start()
        sent.append(size_of(src))

    ready(tok_v)
    ready(mix_v)
    tok = tok_v[...].astype(F32)
    blank = [jnp.zeros((SP - S, depth), F32)] if SP > S else []
    spaced = []
    for k in range(n_kv):
        spaced += [tok[k * S:(k + 1) * S]] + blank
    if n_kv * SP % 16:
        spaced.append(jnp.zeros((16 - n_kv * SP % 16, depth), F32))
    spaced = jnp.concatenate(spaced, axis=0)
    scaled = (spaced * mix_v[...].astype(F32)[None, :]).astype(BF16)
    squares = jnp.sum(spaced * spaced, axis=1, keepdims=True)
    squares = jnp.broadcast_to(squares, (squares.shape[0], 128))
    high = squares.astype(BF16).astype(F32)
    spare = squares - high

    def spread(part, slab, at):
        for k in range(n_kv):
            slab[k, :, at:at + part.shape[1]] = part[k * SP:(k + 1) * SP].astype(BF16)

    spread(high, slab_a, 3 * kcols)
    spread(spare, slab_a, 3 * kcols + 128)
    for at, ref in enumerate((wq_v, wk_v, wd_v)):
        ready(ref)
        spread(jnp.dot(scaled, ref[...], preferred_element_type=F32), slab_a, at * kcols)
    pl.semaphore_wait(barrier, n_kv + n_tp - 2)
    for k in range(n_kv - 1):
        send_kv(slab_a.at[kv_peer(k)], recv_a.at[me], recv_sem.at[0], kv_peer(k))
    ready(wv_v)
    spread(jnp.dot(scaled, wv_v[...], preferred_element_type=F32), slab_v, 0)
    for k in range(n_kv - 1):
        send_kv(slab_v.at[kv_peer(k)], recv_v.at[me], recv_sem.at[1], kv_peer(k))
    ready(wg_v)
    spread(jnp.dot(scaled, wg_v[...], preferred_element_type=F32), slab_g, 0)
    for k in range(n_kv - 1):
        send_kv(slab_g.at[kv_peer(k)], recv_g.at[me], recv_sem.at[2], kv_peer(k))

    ready(len_s)
    ready(decay_v)
    ready(keys_v)
    ready(values_v)
    position = lax.broadcasted_iota(jnp.int32, (positions, kcols), 0)
    befores, weighted = [], []
    for b in range(S):
        length = len_s[b]
        log = decay_v[b]
        before = jnp.sum(jnp.where(position == length - 1, log, 0.0), axis=0, keepdims=True)
        befores.append(before)
        rel = jnp.where(position < length, before - log, -jnp.inf)
        weighted.append((jnp.exp(rel) * keys_v[b].astype(F32)).astype(BF16))
    befores.append(jnp.zeros((8 - S % 8, kcols), F32))
    carry = jnp.transpose(jnp.exp(jnp.concatenate(befores, axis=0)))
    ready(state_v)
    for b in range(S):
        for h in range(heads):
            inner = lax.dot_general(
                weighted[b][:, h * hk:(h + 1) * hk], values_v[b, :, h * hv:(h + 1) * hv],
                (((0,), (0,)), ((), ())), preferred_element_type=F32)
            kept = carry[h * hk:(h + 1) * hk, b:b + 1] * state_v[b, h]
            mat[h, b * hk:(b + 1) * hk, :] = (kept + inner).astype(BF16)
    ready(hg_v)

    def gathered(slab, recv):
        got = slab[me].astype(F32)
        for d in range(1, n_kv):
            got = got + recv[lax.rem(me + d, n_kv)].astype(F32)
        return got

    wait_for(recv_a.at[pl.ds(0, n_kv - 1)], recv_sem.at[0])
    got = gathered(slab_a, recv_a)
    total = got[:, 3 * kcols:3 * kcols + 1] + got[:, 3 * kcols + 128:3 * kcols + 129]
    inverse = lax.rsqrt(total / width + EPSILON)
    query = got[:, :kcols] * inverse * hk ** (-0.5)
    key = got[:, kcols:2 * kcols] * inverse
    x = got[:, 2 * kcols:3 * kcols] * inverse
    log_decay = (jnp.minimum(x, 0.0) - jnp.log1p(jnp.exp(-jnp.abs(x)))) / 16.0
    faded = query * jnp.exp(log_decay)
    product = query * key
    row = lax.broadcasted_iota(jnp.int32, (SP, hk), 0)
    heads_out, owns = [], []
    for h in range(heads):
        cols = slice(h * hk, (h + 1) * hk)
        left = jnp.concatenate(
            [jnp.where(row == b, faded[:, cols], 0.0).astype(BF16) for b in range(S)], axis=1)
        heads_out.append(jnp.dot(left, mat[h], preferred_element_type=F32))
        owns.append(jnp.sum(product[:, cols], axis=1, keepdims=True))

    wait_for(recv_v.at[pl.ds(0, n_kv - 1)], recv_sem.at[1])
    value = gathered(slab_v, recv_v) * inverse
    gain = hg_v[...].astype(F32)[None, :]
    normed = []
    for h in range(heads):
        att = heads_out[h] + owns[h] * value[:, h * hv:(h + 1) * hv]
        normed.append(att * lax.rsqrt(jnp.mean(att * att, axis=1, keepdims=True) + EPSILON) * gain)
    wait_for(recv_g.at[pl.ds(0, n_kv - 1)], recv_sem.at[2])
    gate = gathered(slab_g, recv_g) * inverse
    gate = gate * jax.nn.sigmoid(gate)
    for h in range(heads):
        cols = slice(h * hv, (h + 1) * hv)
        gath[me, :, cols] = (normed[h] * gate[:, cols]).astype(BF16)
    for k in range(n_kv - 1):
        send_kv(gath.at[me], gath.at[me], recv_sem.at[3], kv_peer(k))

    ready(wo_v)
    ready(mg_v)
    wait_for(gath.at[pl.ds(0, n_kv - 1)], recv_sem.at[3])
    merged = jnp.concatenate([gath[k].astype(F32)[:S] for k in range(n_kv)], axis=0).astype(BF16)

    def put(ref, at, part):
        for g in range(part.shape[0] // gs):
            ref[at + (g,)] = part[g * gs:(g + 1) * gs].astype(BF16)

    def get(ref, at, groups):
        return jnp.concatenate([ref[at + (g,)].astype(F32) for g in range(groups)], axis=0)

    def summed(ref, j):
        total = get(ref, (0, j), rows // gs)
        for t in range(1, n_tp):
            total = total + get(ref, (t, j), rows // gs)
        return total

    for j in range(halves):
        put(outx, (mt, j), jnp.dot(merged, wo_v[:, j * dh:(j + 1) * dh], preferred_element_type=F32))
        for d in range(1, n_tp):
            send_tp(outx.at[mt, j], outx.at[mt, j], recv_sem.at[4 + j], d)
    mixed = []
    for j in range(halves):
        wait_for(outx.at[pl.ds(0, n_tp - 1), j], recv_sem.at[4 + j])
        cols = slice(j * dh, (j + 1) * dh)
        mixed.append((tok_v[:, cols].astype(F32) + summed(outx, j)).astype(BF16).astype(F32))
        mlp_lhs[:, cols] = (mixed[j] * mg_v[cols].astype(F32)[None, :]).astype(BF16)
    ready(wu_v)

    def place(p):
        return pl.multiple_of((p // rs) * cw, 128), lax.rem(p, rs) * rr

    def up_of(p):
        col, at = place(p)
        left = mlp_lhs[...] if rs == 1 else mlp_lhs[pl.ds(pl.multiple_of(at, 16), rr), :]
        return jnp.dot(left, wu_v[:, pl.ds(col, cw)], preferred_element_type=F32)

    def up_step(peer, count=1):
        put(up_send, (peer,), up_of(peer))
        send_kv(up_send.at[peer], up_recv.at[me], recv_sem.at[7], peer, count)

    def send_squares():
        lane = lax.broadcasted_iota(jnp.int32, (rows, sq_own.shape[1]), 1)
        at = lax.broadcasted_iota(jnp.int32, (rows, sq_own.shape[1]), 0)
        squares = sum(jnp.sum(m * m, axis=1, keepdims=True) for m in mixed)
        line = jnp.sum(jnp.where(lane == at, squares, 0.0), axis=0, keepdims=True)
        sq_own[...] = jnp.broadcast_to(line, sq_own.shape)
        for k in range(n_kv - 1):
            send_kv(sq_own, sq_recv.at[me], recv_sem.at[6], kv_peer(k))

    if n_kv <= 8:
        for k in range(n_kv - 1):
            up_step(kv_peer(k))
            if k == 0:
                send_squares()
    else:
        send_squares()

        def up_loop(d, carry):
            up_step(lax.rem(me + d, n_kv), n_kv - 1)
            return carry

        lax.fori_loop(1, n_kv, up_loop, 0)
    pre = up_of(me)
    wait_for(sq_recv.at[pl.ds(0, n_kv - 1)], recv_sem.at[6])
    line = sq_own[...]
    for d in range(1, n_kv):
        line = line + sq_recv[lax.rem(me + d, n_kv)]
    lane = lax.broadcasted_iota(jnp.int32, (rows, sq_own.shape[1]), 1)
    at = lax.broadcasted_iota(jnp.int32, (rows, sq_own.shape[1]), 0)
    sq_total = jnp.sum(jnp.where(lane == at, line[:1], 0.0), axis=1, keepdims=True)
    inverse_mlp = lax.rsqrt(sq_total / width + EPSILON)
    if rs > 1:
        sq_mine[...] = jnp.broadcast_to(inverse_mlp, sq_mine.shape)
        inverse_mlp = sq_mine[pl.ds(pl.multiple_of(place(me)[1], 8), rr), :][:, :1]
    wait_for(up_recv.at[pl.ds(0, n_kv - 1)], recv_sem.at[7])
    for d in range(1, n_kv):
        pre = pre + get(up_recv, (lax.rem(me + d, n_kv),), rr // gs)
    act = jnp.maximum(pre * inverse_mlp, 0.0)
    put(sq_all, (me,), act * act)
    for k in range(n_kv - 1):
        send_kv(sq_all.at[me], sq_all.at[me], c_r.at[me], kv_peer(k))
    ready(wdn_v)

    def down_of(p, cols):
        col, at = place(p)
        left = get(sq_all, (p,), rr // gs).astype(BF16)
        return jnp.dot(left, wdn_v[pl.ds(col, cw), cols], preferred_element_type=F32), at

    def arrived(p):
        wait_for(sq_all.at[p], c_r.at[p])

    def ship(j, part):
        put(downx, (mt, j), part)
        for d in range(1, n_tp):
            send_tp(downx.at[mt, j], downx.at[mt, j], recv_sem.at[8 + j], d)

    if rs == 1 and n_kv <= 8:
        acc[...] = down_of(me, slice(None))[0]
        for k in range(n_kv - 2, 0, -1):
            arrived(kv_peer(k))
            acc[...] += down_of(kv_peer(k), slice(None))[0]
        last = kv_peer(0)
        arrived(last)
        for j in range(halves):
            cols = slice(j * dh, (j + 1) * dh)
            ship(j, acc[:, cols] + down_of(last, cols)[0])
    else:
        acc[...] = jnp.zeros_like(acc)

        def add_down(p):
            part, at = down_of(p, slice(None))
            at = pl.ds(pl.multiple_of(at, 8), rr)
            acc[at, :] = acc[at, :] + part

        add_down(me)

        def down_loop(d, carry):
            p = lax.rem(me + d, n_kv)
            arrived(p)
            add_down(p)
            return carry

        lax.fori_loop(1, n_kv, down_loop, 0)
        for j in range(halves):
            ship(j, acc[:, j * dh:(j + 1) * dh])
    for j in range(halves):
        wait_for(downx.at[pl.ds(0, n_tp - 1), j], recv_sem.at[8 + j])
        out[:, j * dh:(j + 1) * dh] = (mixed[j] + summed(downx, j)).astype(BF16)
    tiles = sum(sent) // 2048
    high, wide = wu_v.shape[0] // 8, wu_v.shape[1] // 128
    while tiles:
        fit = [m for m in range(1, wide + 1) if tiles % m == 0 and tiles // m <= high]
        m = max(fit) if fit else wide
        r = min(tiles // m, high)
        wait_for(wu_v.at[pl.ds(0, 8 * r), pl.ds(0, 128 * m)], send_sem.at[0])
        tiles -= r * m


def on_device(n_kv, n_tp, *args):
    tokens, wq, wv, state, keys, wu, wdn = (args[i] for i in (0, 2, 5, 7, 8, 15, 16))
    rows, depth = tokens.shape
    S, heads, hk, hv = state.shape
    SP = (S + 3) // 4 * 4
    kcols, vcols, hidden = wq.shape[1], wv.shape[1], wu.shape[1]
    col_splits = min(n_kv, hidden // 128)
    rs = n_kv // col_splits
    rr, cw = rows // rs, hidden // col_splits
    gs = 8 if rr % 8 == 0 else 4
    halves = 2 if depth % 256 == 0 else 1
    dh = depth // halves
    lanes = (rows + 127) // 128 * 128
    loaded = [args[i] for i in (0, 1, 2, 3, 4, 5, 6, 7, 8, 9, 10)]
    later = [args[i] for i in (12, 13, 14, 15, 16)]
    V = pltpu.VMEM
    wa = 3 * kcols + 256
    shared = V((n_tp, halves, rows // gs, gs, dh), BF16)
    hidden_part = V((n_kv, rr // gs, gs, cw), BF16)
    scratch = (
        [V(a.shape, a.dtype) for a in loaded] + [pltpu.SMEM(args[11].shape, args[11].dtype)]
        + [V(a.shape, a.dtype) for a in later] + [
            V((n_kv, SP, wa), BF16), V((n_kv, SP, vcols), BF16), V((n_kv, SP, vcols), BF16),
            V((n_kv, SP, wa), BF16), V((n_kv, SP, vcols), BF16), V((n_kv, SP, vcols), BF16),
            V((n_kv, SP, vcols), BF16), shared,
            V((4, lanes), F32), V((n_kv, 4, lanes), F32), V((rows, depth), BF16),
            hidden_part, hidden_part, V((rows, 128), F32),
            hidden_part, V((rows, depth), F32), shared,
            V((heads, S * hk, hv), BF16),
            pltpu.SemaphoreType.DMA((17,)), pltpu.SemaphoreType.DMA((1,)),
            pltpu.SemaphoreType.DMA((8 + halves,)), pltpu.SemaphoreType.DMA((n_kv,)),
        ])
    cfg = (n_kv, n_tp, depth * n_kv, S, SP, rs, gs, halves)
    return pl.pallas_call(
        functools.partial(kernel, cfg),
        out_shape=pltpu.VMEM((rows, depth), BF16),
        in_specs=[ANY] * 17,
        out_specs=pl.BlockSpec(memory_space=pltpu.VMEM),
        scratch_shapes=scratch,
        compiler_params=pltpu.CompilerParams(
            collective_id=0, has_side_effects=True, vmem_limit_bytes=60 * 1024 * 1024),
    )(*args)


def solution(mesh):
    return jax.shard_map(
        functools.partial(on_device, mesh.shape["kv"], mesh.shape["tp"]),
        mesh=mesh,
        in_specs=(
            P("grp", "kv"),
            P("kv"),
            P("kv", "tp"),
            P("kv", "tp"),
            P("kv", "tp"),
            P("kv", "tp"),
            P("kv", "tp"),
            P(("grp", "kv"), "tp", None, None),
            P(("grp", "kv"), None, "tp"),
            P(("grp", "kv"), None, "tp"),
            P(("grp", "kv"), None, "tp"),
            P(("grp", "kv")),
            P(),
            P("tp", "kv"),
            P("kv"),
            P("kv", "tp"),
            P("tp", "kv"),
        ),
        out_specs=P("grp", "kv"),
        check_vma=False,
    )
```
